32 devices in a mesh: dp: 2 (over x), kv: 8 (over z, y), tp: 2 (over core).
Axes of the slice: x: 2, y: 2, z: 4, core: 2. Of those that a mesh axis runs over, the one named last changes fastest.
Arguments:
- tokens: bfloat16 [32, 3072], P(('tp', 'dp'), 'kv'), parts along dimension 0, may hold values from -60 to 60
- old_state: float32 [32, 24, 128, 128], P(('tp', 'dp', 'kv')), parts along dimension 0, may hold values from -0.6 to 0.6
- mixer_gain: float32 [3072], replicated, may hold values from 0.1 to 1.9
- w_query: bfloat16 [3072, 3072], P(None, 'kv'), may hold values from -0.109375 to 0.109375
- w_key: bfloat16 [3072, 3072], P(None, 'kv'), may hold values from -0.109375 to 0.109375
- w_value: bfloat16 [3072, 3072], P(None, 'kv'), may hold values from -0.109375 to 0.109375
- w_outgate: bfloat16 [3072, 3072], P(None, 'kv'), may hold values from -0.109375 to 0.109375
- w_decay: bfloat16 [3072, 24], replicated, may hold values from -0.109375 to 0.109375
- w_write: bfloat16 [3072, 24], replicated, may hold values from -0.109375 to 0.109375
- decay_log: float32 [24], replicated, may hold values from -3 to 1
- decay_bias: float32 [24], replicated, may hold values from -3 to 3
- head_gain: float32 [128], replicated, may hold values from 0.1 to 1.9
- w_output: bfloat16 [3072, 3072], P('kv'), may hold values from -0.15625 to 0.15625
- channel_gain: float32 [3072], replicated, may hold values from 0.1 to 1.9
- w_gate: bfloat16 [3072, 8448], P(None, 'kv'), may hold values from -0.109375 to 0.109375
- w_up: bfloat16 [3072, 8448], P(None, 'kv'), may hold values from -0.109375 to 0.109375
- w_down: bfloat16 [8448, 3072], P(None, 'kv'), may hold values from -0.0625 to 0.0625
Outputs:
- mixed: bfloat16 [32, 3072], P(('tp', 'dp'), 'kv'), parts along dimension 0
- new_state: float32 [32, 24, 128, 128], P(('tp', 'dp', 'kv')), parts along dimension 0
The draws below stay inside these ranges and needn't reach their ends.
There are 2 independent parts, one for each index of `tp`. The reference program is written for one: setup_inputs(seed, part) draws one part's arguments, and reference() takes and returns one part's arrays. A program takes and returns all parts, laid end to end along the dimension named above; an argument that names none is the same for every part. Nothing has to cross between parts.
All inputs are finite; a program needn't handle non-finite values.
Results may differ from the reference program's by a relative error of at most 0.0059.
Values may be sent and summed in bfloat16 or wider, within the bound.
A program may use at most 64 MiB of HBM per device.

```python
import jax
import jax.numpy as jnp
from jax import lax

D = 3072
HEADS = 24
HEAD_DIM = 128
FF = 8448
BATCH = 16


def draw_tokens(key, part):
    row_key, rough_key, normal_key = jax.random.split(key, 3)
    row_scale = jnp.exp(jax.random.uniform(row_key, (BATCH, 1), jnp.float32, jnp.log(0.3), jnp.log(3.0)))
    position_ramp = jnp.arange(D, dtype=jnp.float32) / D
    rough_factor = jax.random.uniform(rough_key, (D,), jnp.float32, 0.6, 1.4)
    column_scale = jnp.exp(jnp.log(0.4) + jnp.log(8.0) * position_ramp) * rough_factor
    normal_part = jax.random.truncated_normal(normal_key, -4.0, 4.0, (BATCH, D), jnp.float32)
    return (normal_part * row_scale * column_scale[None, :]).astype(jnp.bfloat16)


def spiked(entries, key, source, target, parts, factor):
    owner, partner = [(jnp.arange(entries.shape[dim]) // (entries.shape[dim] // parts)).reshape([-1 if axis == dim else 1 for axis in range(entries.ndim)]) for dim in (source, target)]
    chosen = jax.random.permutation(key, parts)[partner]
    strong = (owner == chosen) | (owner == (partner + parts // 2) % parts)
    return jnp.where(strong, factor * entries, entries)


def level_of(key, shape, cuts, least, top_value):
    def one(position, parts):
        heights = jax.random.uniform(jax.random.fold_in(jax.random.fold_in(key, 6), position), (parts,), jnp.float32, least / len(cuts), top_value / len(cuts))
        return jnp.repeat(jnp.exp(heights), shape[position] // parts).reshape((-1,) + (1,) * (len(shape) - position - 1))

    level = one(*cuts[0])
    for cut in cuts[1:]:
        level = level * one(*cut)
    return level


def gaussian(rng, dims, scale, most, pieces=(), kind=jnp.bfloat16):
    values = jax.random.normal(rng, dims, jnp.float32) * scale
    if len(pieces) > 0:
        values = level_of(rng, dims, pieces, -0.22, 0.18) * values
    return jnp.clip(values, min=-most, max=most).astype(kind)


def bell_draw_with(key, extent, scale, limit, pieces, heavy, kind=jnp.bfloat16):
    values = scale * jax.random.normal(key, extent, jnp.float32)
    if pieces:
        values = values * level_of(key, extent, pieces, -0.22, 0.18)
    return jnp.clip(spiked(values, jax.random.fold_in(key, 3), *heavy), -limit, limit).astype(kind)


def setup_inputs(seed: int = 0, part: int = 0) -> dict:
    keys = jax.random.split(jax.random.key(seed), 18)
    own_keys = jax.random.split(jax.random.fold_in(keys[17], part), 18)
    return {
        "tokens": draw_tokens(jax.random.fold_in(jax.random.fold_in(keys[17], part), 71), part),
        "old_state": gaussian(own_keys[1], (BATCH, HEADS, HEAD_DIM, HEAD_DIM), 0.1, 0.6, ((0, 16),), jnp.float32),
        "mixer_gain": jnp.clip(1.0 + 0.18 * jax.random.normal(keys[2], (D,), jnp.float32), 0.1, 1.9),
        "w_query": gaussian(keys[3], (D, HEADS * HEAD_DIM), D ** -0.5, 0.109375, ((1, 8),)),
        "w_key": gaussian(keys[4], (D, HEADS * HEAD_DIM), D ** -0.5, 0.109375, ((1, 8),)),
        "w_value": gaussian(keys[5], (D, HEADS * HEAD_DIM), D ** -0.5, 0.109375, ((1, 8),)),
        "w_outgate": gaussian(keys[6], (D, HEADS * HEAD_DIM), D ** -0.5, 0.109375, ((1, 8),)),
        "w_decay": gaussian(keys[7], (D, HEADS), D ** -0.5, 0.109375),
        "w_write": gaussian(keys[8], (D, HEADS), D ** -0.5, 0.109375),
        "decay_log": jnp.clip(jax.random.uniform(keys[9], (HEADS,), jnp.float32, -3.0, 1.0), -3.0, 1.0),
        "decay_bias": gaussian(keys[10], (HEADS,), 1.0, 3.0, (), jnp.float32),
        "head_gain": jnp.clip(1.0 + 0.18 * jax.random.normal(keys[11], (HEAD_DIM,), jnp.float32), 0.1, 1.9),
        "w_output": bell_draw_with(keys[12], (HEADS * HEAD_DIM, D), (HEADS * HEAD_DIM) ** -0.5, 0.15625, ((0, 8),), (0, 1, 8, 2.0)),
        "channel_gain": jnp.clip(1.0 + 0.18 * jax.random.normal(keys[13], (D,), jnp.float32), 0.1, 1.9),
        "w_gate": gaussian(keys[14], (D, FF), D ** -0.5, 0.109375, ((1, 8),)),
        "w_up": gaussian(keys[15], (D, FF), D ** -0.5, 0.109375, ((1, 8),)),
        "w_down": gaussian(keys[16], (FF, D), FF ** -0.5, 0.0625, ((1, 8),)),
    }


EPS = 1e-06

def norm_scale(values):
    return lax.rsqrt(lax.optimization_barrier(jnp.mean(values * values, axis=-1, keepdims=True)) + EPS)

def unit_rows(values):
    return values * lax.rsqrt(lax.optimization_barrier(jnp.sum(values * values, axis=-1, keepdims=True)) + EPS)

def sequence_update(packed_blocks):
    previous_state, query_vector, key_vector, value_vec, retain, strength = packed_blocks
    recalled_values = jnp.einsum('gfy,gf->gy', previous_state, key_vector, precision=lax.Precision.HIGHEST)
    correction = value_vec - retain[:, None] * recalled_values
    updated_state = retain[:, None, None] * previous_state + (strength[:, None] * key_vector)[:, :, None] * correction[:, None, :]
    state_readout = jnp.einsum('gfy,gf->gy', updated_state, query_vector, precision=lax.Precision.HIGHEST)
    return (updated_state, state_readout)

def reference(tokens, old_state, mixer_gain, w_query, w_key, w_value, w_outgate, w_decay, w_write, decay_log, decay_bias, head_gain, w_output, channel_gain, w_gate, w_up, w_down):
    batch_rows = tokens.shape[0]
    tok_wide = tokens.astype(jnp.float32)
    scale_in = norm_scale(tok_wide)
    normed = (tok_wide * mixer_gain).astype(jnp.bfloat16)

    def project(weight):
        return jnp.dot(normed, weight, preferred_element_type=jnp.float32) * scale_in

    def by_head(values):
        return values.astype(jnp.float32).reshape(batch_rows, HEADS, HEAD_DIM)
    query_pre = project(w_query).astype(jnp.bfloat16)
    key_pre = project(w_key).astype(jnp.bfloat16)
    value_pre = project(w_value).astype(jnp.bfloat16)
    outgate_pre = project(w_outgate).astype(jnp.bfloat16)
    decay_pre = project(w_decay)
    write_pre = project(w_write)
    queries = unit_rows(jax.nn.silu(by_head(query_pre))) * HEAD_DIM ** (-0.5)
    keys_unit = unit_rows(jax.nn.silu(by_head(key_pre)))
    values_act = jax.nn.silu(by_head(value_pre))
    strength = jax.nn.sigmoid(write_pre)
    retain = jnp.exp(-jnp.exp(decay_log) * jax.nn.softplus(decay_pre + decay_bias))
    new_state, state_readout = lax.map(sequence_update, (old_state, queries, keys_unit, values_act, retain, strength))
    gated_read = state_readout * norm_scale(state_readout) * head_gain * jax.nn.silu(by_head(outgate_pre))
    gated_read = gated_read.reshape(batch_rows, HEADS * HEAD_DIM).astype(jnp.bfloat16)
    mixer_out = jnp.dot(gated_read, w_output, preferred_element_type=jnp.float32)
    residual = lax.optimization_barrier((tok_wide + mixer_out).astype(jnp.bfloat16))
    residual_wide = residual.astype(jnp.float32)
    scale_mid = norm_scale(residual_wide)
    normed_mid = (residual_wide * channel_gain).astype(jnp.bfloat16)
    gate_act = jnp.dot(normed_mid, w_gate, preferred_element_type=jnp.float32) * scale_mid
    upward = jnp.dot(normed_mid, w_up, preferred_element_type=jnp.float32) * scale_mid
    hidden_units = (jax.nn.silu(gate_act) * upward).astype(jnp.bfloat16)
    down_sum = jnp.dot(hidden_units, w_down, preferred_element_type=jnp.float32)
    mixed = (residual_wide + down_sum).astype(jnp.bfloat16)
    return (mixed, new_state)
```

```python
import functools

import jax
import jax.numpy as jnp
from jax import lax
from jax.experimental import pallas as pl
from jax.experimental.pallas import tpu as pltpu
from jax.sharding import PartitionSpec as P

MESH = pl.DeviceIdType.MESH
F32 = jnp.float32
BF16 = jnp.bfloat16

HEADS = 24
HEAD_DIM = 128


EPS = 1e-06


def norm_scale(values):
    return lax.rsqrt(jnp.mean(values * values, axis=-1, keepdims=True) + EPS)


def unit_rows(values):
    return values * lax.rsqrt(jnp.sum(values * values, axis=-1, keepdims=True) + EPS)


def body(
    tokens,
    old_state,
    mixer_gain,
    w_query,
    w_key,
    w_value,
    w_outgate,
    w_decay,
    w_write,
    decay_log,
    decay_bias,
    head_gain,
    w_output,
    channel_gain,
    w_gate,
    w_up,
    w_down,
):
    local_rows = old_state.shape[0]
    width_share = tokens.shape[1]
    offset_rows = lax.axis_index("kv") * local_rows
    offset_cols = lax.axis_index("kv") * width_share
    complete_rows = lax.all_gather(tokens, "kv", axis=1, tiled=True)
    tok_wide = complete_rows.astype(jnp.float32)
    scale_in = norm_scale(tok_wide)
    normed = (tok_wide * mixer_gain).astype(jnp.bfloat16)

    def project(weight):
        return (jnp.dot(normed, weight, preferred_element_type=jnp.float32) * scale_in).astype(
            jnp.bfloat16
        )

    query_cols = project(w_query)
    key_cols = project(w_key)
    value_cols = project(w_value)
    outgate_cols = project(w_outgate)
    query_pre, key_pre, value_pre, outgate_pre = (
        lax.all_to_all(query_cols, "kv", split_axis=0, concat_axis=1, tiled=True),
        lax.all_to_all(key_cols, "kv", split_axis=0, concat_axis=1, tiled=True),
        lax.all_to_all(value_cols, "kv", split_axis=0, concat_axis=1, tiled=True),
        lax.all_to_all(outgate_cols, "kv", split_axis=0, concat_axis=1, tiled=True),
    )
    own_normed = lax.dynamic_slice_in_dim(normed, offset_rows, local_rows, 0)
    own_scale = lax.dynamic_slice_in_dim(scale_in, offset_rows, local_rows, 0)
    decay_pre = jnp.dot(own_normed, w_decay, preferred_element_type=jnp.float32) * own_scale
    write_pre = jnp.dot(own_normed, w_write, preferred_element_type=jnp.float32) * own_scale

    def by_head(values):
        return values.astype(jnp.float32).reshape(local_rows, HEADS, HEAD_DIM)

    queries = unit_rows(jax.nn.silu(by_head(query_pre))) * HEAD_DIM ** (-0.5)
    keys_unit = unit_rows(jax.nn.silu(by_head(key_pre)))
    values_act = jax.nn.silu(by_head(value_pre))
    strength = jax.nn.sigmoid(write_pre)
    retain = jnp.exp(-jnp.exp(decay_log) * jax.nn.softplus(decay_pre + decay_bias))
    recalled_values = jnp.einsum(
        "bhkv,bhk->bhv", old_state, keys_unit, precision=lax.Precision.HIGHEST
    )
    correction = values_act - retain[..., None] * recalled_values
    new_state = (
        retain[..., None, None] * old_state
        + (strength[..., None] * keys_unit)[..., :, None] * correction[..., None, :]
    )
    state_readout = jnp.einsum("bhkv,bhk->bhv", new_state, queries, precision=lax.Precision.HIGHEST)
    gated_read = (
        state_readout * norm_scale(state_readout) * head_gain * jax.nn.silu(by_head(outgate_pre))
    )
    gated_read = gated_read.reshape(local_rows, HEADS * HEAD_DIM).astype(jnp.bfloat16)
    read_cols = lax.all_to_all(gated_read, "kv", split_axis=1, concat_axis=0, tiled=True)
    partial_out = jnp.dot(read_cols, w_output, preferred_element_type=jnp.float32)
    mixer_out = lax.psum(partial_out, "kv")
    residual = lax.optimization_barrier((tok_wide + mixer_out).astype(jnp.bfloat16))
    residual_wide = residual.astype(jnp.float32)
    scale_mid = norm_scale(residual_wide)
    normed_mid = (residual_wide * channel_gain).astype(jnp.bfloat16)
    gate_act = jnp.dot(normed_mid, w_gate, preferred_element_type=jnp.float32) * scale_mid
    upward = jnp.dot(normed_mid, w_up, preferred_element_type=jnp.float32) * scale_mid
    own_residual = lax.dynamic_slice_in_dim(residual_wide, offset_cols, width_share, 1)
    hidden_units = (jax.nn.silu(gate_act) * upward).astype(jnp.bfloat16)
    down_sum = jnp.dot(
        lax.all_gather(hidden_units, "kv", axis=1, tiled=True),
        w_down,
        preferred_element_type=jnp.float32,
    )
    mixed = (own_residual + down_sum).astype(jnp.bfloat16)
    return (mixed, new_state)


TOKENS, PRE, READ, PARTIAL, RESIDUAL, HIDDEN = range(6)


def silu(values):
    return values / (1.0 + jnp.exp(-values))


def layer_kernel(
    n,
    depth_tile,
    tok_ref,
    mixer_gain_ref,
    decay_log_ref,
    decay_bias_ref,
    head_gain_ref,
    channel_gain_ref,
    w_query,
    w_key,
    w_value,
    w_outgate,
    w_decay,
    w_write,
    old_state,
    w_output,
    w_gate,
    w_up,
    w_down,
    mixed_ref,
    new_state,
    v_query,
    v_key,
    v_value,
    v_outgate,
    v_decay,
    v_write,
    v_state,
    v_output,
    v_gate,
    v_up,
    v_down,
    tok_all,
    normed,
    small,
    pre_out,
    pre_in,
    head_rows,
    head_vals,
    head_gate,
    read_rows,
    read_out,
    read_in,
    part_out,
    part_in,
    res_own,
    res_all,
    hid_own,
    hid_all,
    sem_proj,
    sem_small,
    sem_mix,
    sem_down,
    send_sem,
    recv_sem,
):
    me = lax.axis_index("kv")
    rows, share = tok_ref.shape
    local_rows, heads = v_state.shape[0], v_state.shape[1]
    width = n * share
    own_heads = share // HEAD_DIM
    hidden_share = v_gate.shape[1]
    steps = width // depth_tile

    barrier = pltpu.get_barrier_semaphore()
    for k in range(1, n):
        pl.semaphore_signal(
            barrier, inc=1, device_id={"kv": lax.rem(me + k, n)}, device_id_type=MESH
        )

    proj = ((w_query, v_query), (w_key, v_key), (w_value, v_value), (w_outgate, v_outgate))
    mix = ((w_gate, v_gate), (w_up, v_up))

    def tile_copy(pair, step, sem):
        part = pl.ds(pl.multiple_of(step * depth_tile, depth_tile), depth_tile)
        return pltpu.make_async_copy(pair[0].at[part], pair[1].at[part], sem)

    def proj_copy(which, step):
        return tile_copy(proj[which], step, sem_proj.at[step, which])

    def mix_copy(which, step):
        return tile_copy(mix[which], step, sem_mix.at[step, which])

    def down_copy(step):
        part = pl.ds(pl.multiple_of(step * hidden_share, 16), hidden_share)
        return pltpu.make_async_copy(w_down.at[part], v_down.at[part], sem_down.at[step])

    decay_copy = pltpu.make_async_copy(w_decay, v_decay, sem_small.at[0])
    write_copy = pltpu.make_async_copy(w_write, v_write, sem_small.at[1])
    state_copy = pltpu.make_async_copy(old_state, v_state, sem_small.at[2])
    output_copy = pltpu.make_async_copy(w_output, v_output, sem_small.at[3])
    decay_copy.start()
    write_copy.start()
    for step in range(steps):
        for which in range(4):
            proj_copy(which, step).start()

    pl.semaphore_wait(barrier, n - 1)

    def exchange(phase, source, slots):
        copies = []
        for k in range(1, n):
            peer = lax.rem(me + k, n)
            copy = pltpu.make_async_remote_copy(
                src_ref=source(peer),
                dst_ref=slots.at[me],
                send_sem=send_sem.at[phase, k],
                recv_sem=recv_sem.at[phase, k],
                device_id={"kv": peer},
                device_id_type=MESH,
            )
            copy.start()
            copies.append(copy)
        return copies

    def arrive(copies):
        for copy in copies:
            copy.wait_recv()

    all_copies = []

    copies = exchange(TOKENS, lambda peer: tok_ref, tok_all)
    all_copies += copies
    state_copy.start()
    output_copy.start()
    for step in range(steps):
        for which in range(2):
            mix_copy(which, step).start()
    for step in range(n):
        down_copy(step).start()
    tok_all[me] = tok_ref[...]
    if pre_out.shape[1] > 4 * own_heads:
        pre_out[:, 4 * own_heads :, :] = jnp.zeros(
            (rows, pre_out.shape[1] - 4 * own_heads, HEAD_DIM), F32
        )
    read_out[...] = jnp.zeros_like(read_out)
    head_rows[...] = jnp.zeros_like(head_rows)
    arrive(copies)

    def norm_into(blocks, gain_ref):
        squares = jnp.zeros((rows, 1), F32)
        for s in range(n):
            cols = slice(s * share, (s + 1) * share)
            wide = blocks[s].astype(F32)
            squares += jnp.sum(wide * wide, axis=-1, keepdims=True)
            normed[:, cols] = (wide * gain_ref[:, cols]).astype(BF16)
        return lax.rsqrt(squares / width + EPS)

    scale_in = norm_into(tok_all, mixer_gain_ref)

    decay_copy.wait()
    write_copy.wait()

    def proj_step(step, sums):
        part = pl.ds(pl.multiple_of(step * depth_tile, depth_tile), depth_tile)
        lhs = normed[:, part]
        out = []
        for which in range(4):
            proj_copy(which, step).wait()
            out.append(
                sums[which]
                + jnp.dot(lhs, proj[which][1][part, :], preferred_element_type=F32)
            )
        out.append(sums[4] + jnp.dot(lhs, v_decay[part, :], preferred_element_type=F32))
        out.append(sums[5] + jnp.dot(lhs, v_write[part, :], preferred_element_type=F32))
        return tuple(out)

    zeros = lambda cols: jnp.zeros((rows, cols), F32)
    sums = lax.fori_loop(
        0, steps, proj_step, (zeros(share),) * 4 + (zeros(heads),) * 2
    )
    for which in range(4):
        pre = (sums[which] * scale_in).astype(BF16).astype(F32)
        for j in range(own_heads):
            pre_out[:, which * own_heads + j, :] = pre[:, j * HEAD_DIM : (j + 1) * HEAD_DIM]

    def row_block(peer):
        return pre_out.at[pl.ds(peer * local_rows, local_rows)]

    copies = exchange(PRE, row_block, pre_in)
    all_copies += copies
    pre_in[me] = pre_out[pl.ds(me * local_rows, local_rows)]
    small[0] = sums[4] * scale_in
    small[1] = sums[5] * scale_in
    state_copy.wait()
    arrive(copies)

    for l in range(local_rows):
        own = pl.ds(me * local_rows + l, 1)
        decay_pre = small[0, own, :]
        write_pre = small[1, own, :]
        strength = 1.0 / (1.0 + jnp.exp(-write_pre))
        shifted = decay_pre + decay_bias_ref[...]
        softplus = jnp.maximum(shifted, 0.0) + jnp.log1p(jnp.exp(-jnp.abs(shifted)))
        retain = jnp.exp(-jnp.exp(decay_log_ref[...]) * softplus)
        for s in range(n):
            act = silu(pre_in[s, l])
            unit = act * lax.rsqrt(jnp.sum(act * act, axis=-1, keepdims=True) + EPS)
            at = s * own_heads
            c = own_heads
            head_rows[at : at + c, :] = unit[c : 2 * c]
            head_rows[heads + at : heads + at + c, :] = unit[:c] * HEAD_DIM ** (-0.5)
            head_vals[at : at + c, :] = act[2 * c : 3 * c]
            head_gate[at : at + c, :] = act[3 * c : 4 * c]
        columns = head_rows[...].T
        for h in range(heads):
            key = columns[:, h : h + 1]
            query = columns[:, heads + h : heads + h + 1]
            keep = retain[:, h : h + 1]
            old = v_state[l, h]
            recalled = jnp.sum(old * key, axis=0, keepdims=True)
            correction = head_vals[h : h + 1, :] - keep * recalled
            new = keep * old + key * (strength[:, h : h + 1] * correction)
            v_state[l, h] = new
            read_rows[h : h + 1, :] = jnp.sum(new * query, axis=0, keepdims=True)
        read = read_rows[...]
        scale = lax.rsqrt(jnp.mean(read * read, axis=-1, keepdims=True) + EPS)
        gated = (read * scale * head_gain_ref[...] * head_gate[...]).astype(BF16).astype(F32)
        for s in range(n):
            read_out[s, l, :own_heads, :] = gated[s * own_heads : (s + 1) * own_heads]

    copies = exchange(READ, lambda peer: read_out.at[peer], read_in)
    all_copies += copies
    state_out = pltpu.make_async_copy(v_state, new_state, sem_small.at[4])
    state_out.start()
    read_in[me] = read_out[me]
    output_copy.wait()
    arrive(copies)
    read_cols = jnp.concatenate(
        [read_in[:, :, j, :].reshape(rows, HEAD_DIM) for j in range(own_heads)], axis=1
    ).astype(BF16)
    for s in range(n):
        part_out[s] = jnp.dot(
            read_cols, v_output[:, s * share : (s + 1) * share], preferred_element_type=F32
        )

    copies = exchange(PARTIAL, lambda peer: part_out.at[peer], part_in)
    all_copies += copies
    part_in[me] = part_out[me]
    arrive(copies)
    residual = tok_ref[...].astype(F32)
    mixer = part_in[0]
    for s in range(1, n):
        mixer += part_in[s]
    res_own[...] = (residual + mixer).astype(BF16)
    copies = exchange(RESIDUAL, lambda peer: res_own, res_all)
    all_copies += copies
    res_all[me] = res_own[...]
    arrive(copies)
    scale_mid = norm_into(res_all, channel_gain_ref)

    def mix_step(step, sums):
        part = pl.ds(pl.multiple_of(step * depth_tile, depth_tile), depth_tile)
        lhs = normed[:, part]
        out = []
        for which in range(2):
            mix_copy(which, step).wait()
            out.append(
                sums[which] + jnp.dot(lhs, mix[which][1][part, :], preferred_element_type=F32)
            )
        return tuple(out)

    gate, up = lax.fori_loop(0, steps, mix_step, (zeros(hidden_share),) * 2)
    hid_own[...] = (silu(gate * scale_mid) * (up * scale_mid)).astype(BF16)

    copies = exchange(HIDDEN, lambda peer: hid_own, hid_all)
    all_copies += copies
    hid_all[me] = hid_own[...]
    arrive(copies)

    def down_step(step, total):
        down_copy(step).wait()
        part = pl.ds(pl.multiple_of(step * hidden_share, 16), hidden_share)
        return total + jnp.dot(hid_all[step], v_down[part, :], preferred_element_type=F32)

    total = lax.fori_loop(0, n, down_step, zeros(share))
    mixed_ref[...] = (res_own[...].astype(F32) + total).astype(BF16)

    for copy in all_copies:
        copy.wait_send()
    state_out.wait()


def round_up(value, unit):
    return -(-value // unit) * unit


def fused_body(
    n,
    tokens,
    old_state,
    mixer_gain,
    w_query,
    w_key,
    w_value,
    w_outgate,
    w_decay,
    w_write,
    decay_log,
    decay_bias,
    head_gain,
    w_output,
    channel_gain,
    w_gate,
    w_up,
    w_down,
):
    rows, share = tokens.shape
    local_rows, heads = old_state.shape[:2]
    width, hidden_share = w_gate.shape
    own_heads = share // HEAD_DIM
    depth_tile = 512 if width % 512 == 0 else share
    steps = width // depth_tile
    pre_rows = round_up(4 * own_heads, 8)
    read_slots = round_up(own_heads, 8)
    vmem = pl.BlockSpec(memory_space=pltpu.VMEM)
    hbm = pl.BlockSpec(memory_space=pl.ANY)
    buf = pltpu.VMEM
    sem = pltpu.SemaphoreType.DMA
    wide = lambda vector: vector.reshape(1, -1)
    return tuple(
        pl.pallas_call(
            functools.partial(layer_kernel, n, depth_tile),
            out_shape=(
                jax.ShapeDtypeStruct((rows, share), BF16),
                jax.ShapeDtypeStruct(old_state.shape, F32),
            ),
            in_specs=[vmem] * 6 + [hbm] * 11,
            out_specs=(vmem, hbm),
            scratch_shapes=[
                buf((width, share), BF16),
                buf((width, share), BF16),
                buf((width, share), BF16),
                buf((width, share), BF16),
                buf(w_decay.shape, BF16),
                buf(w_write.shape, BF16),
                buf(old_state.shape, F32),
                buf(w_output.shape, BF16),
                buf(w_gate.shape, BF16),
                buf(w_up.shape, BF16),
                buf(w_down.shape, BF16),
                buf((n, rows, share), BF16),
                buf((rows, width), BF16),
                buf((2, rows, heads), F32),
                buf((rows, pre_rows, HEAD_DIM), F32),
                buf((n, local_rows, pre_rows, HEAD_DIM), F32),
                buf((round_up(2 * heads, 128), HEAD_DIM), F32),
                buf((heads, HEAD_DIM), F32),
                buf((heads, HEAD_DIM), F32),
                buf((heads, HEAD_DIM), F32),
                buf((n, local_rows, read_slots, HEAD_DIM), F32),
                buf((n, local_rows, read_slots, HEAD_DIM), F32),
                buf((n, rows, share), F32),
                buf((n, rows, share), F32),
                buf((rows, share), BF16),
                buf((n, rows, share), BF16),
                buf((rows, hidden_share), BF16),
                buf((n, rows, hidden_share), BF16),
                sem((steps, 4)),
                sem((5,)),
                sem((steps, 2)),
                sem((n,)),
                sem((6, n)),
                sem((6, n)),
            ],
            compiler_params=pltpu.CompilerParams(
                collective_id=0, has_side_effects=True, vmem_limit_bytes=63 * 2**20
            ),
        )(
            tokens,
            wide(mixer_gain),
            wide(decay_log),
            wide(decay_bias),
            wide(head_gain),
            wide(channel_gain),
            w_query,
            w_key,
            w_value,
            w_outgate,
            w_decay,
            w_write,
            old_state,
            w_output,
            w_gate,
            w_up,
            w_down,
        )
    )


def any_body(n, tokens, old_state, *rest):
    whole_heads = tokens.shape[1] % HEAD_DIM == 0 and tokens.shape[0] % 8 == 0
    held = sum(a.size * a.dtype.itemsize for a in (old_state, *rest))
    if whole_heads and held < 40 * 2**20:
        return fused_body(n, tokens, old_state, *rest)
    return body(tokens, old_state, *rest)


def solution(mesh):
    in_specs = (
        P(("tp", "dp"), "kv"),
        P(("tp", "dp", "kv"), None, None, None),
        P(),
        P(None, "kv"),
        P(None, "kv"),
        P(None, "kv"),
        P(None, "kv"),
        P(),
        P(),
        P(),
        P(),
        P(),
        P("kv", None),
        P(),
        P(None, "kv"),
        P(None, "kv"),
        P(None, "kv"),
    )
    out_specs = (P(("tp", "dp"), "kv"), P(("tp", "dp", "kv"), None, None, None))
    return jax.shard_map(
        functools.partial(any_body, mesh.shape["kv"]), mesh=mesh, in_specs=in_specs, out_specs=out_specs, check_vma=False)
```

```python
import functools

import jax
import jax.numpy as jnp
from jax import lax
from jax.experimental import pallas as pl
from jax.experimental.pallas import tpu as pltpu
from jax.sharding import PartitionSpec as P

MESH = pl.DeviceIdType.MESH
F32 = jnp.float32
BF16 = jnp.bfloat16

HEADS = 24
HEAD_DIM = 128


EPS = 1e-06


def norm_scale(values):
    return lax.rsqrt(jnp.mean(values * values, axis=-1, keepdims=True) + EPS)


def unit_rows(values):
    return values * lax.rsqrt(jnp.sum(values * values, axis=-1, keepdims=True) + EPS)


def body(
    tokens,
    old_state,
    mixer_gain,
    w_query,
    w_key,
    w_value,
    w_outgate,
    w_decay,
    w_write,
    decay_log,
    decay_bias,
    head_gain,
    w_output,
    channel_gain,
    w_gate,
    w_up,
    w_down,
):
    local_rows = old_state.shape[0]
    width_share = tokens.shape[1]
    offset_rows = lax.axis_index("kv") * local_rows
    offset_cols = lax.axis_index("kv") * width_share
    complete_rows = lax.all_gather(tokens, "kv", axis=1, tiled=True)
    tok_wide = complete_rows.astype(jnp.float32)
    scale_in = norm_scale(tok_wide)
    normed = (tok_wide * mixer_gain).astype(jnp.bfloat16)

    def project(weight):
        return (jnp.dot(normed, weight, preferred_element_type=jnp.float32) * scale_in).astype(
            jnp.bfloat16
        )

    query_cols = project(w_query)
    key_cols = project(w_key)
    value_cols = project(w_value)
    outgate_cols = project(w_outgate)
    query_pre, key_pre, value_pre, outgate_pre = (
        lax.all_to_all(query_cols, "kv", split_axis=0, concat_axis=1, tiled=True),
        lax.all_to_all(key_cols, "kv", split_axis=0, concat_axis=1, tiled=True),
        lax.all_to_all(value_cols, "kv", split_axis=0, concat_axis=1, tiled=True),
        lax.all_to_all(outgate_cols, "kv", split_axis=0, concat_axis=1, tiled=True),
    )
    own_normed = lax.dynamic_slice_in_dim(normed, offset_rows, local_rows, 0)
    own_scale = lax.dynamic_slice_in_dim(scale_in, offset_rows, local_rows, 0)
    decay_pre = jnp.dot(own_normed, w_decay, preferred_element_type=jnp.float32) * own_scale
    write_pre = jnp.dot(own_normed, w_write, preferred_element_type=jnp.float32) * own_scale

    def by_head(values):
        return values.astype(jnp.float32).reshape(local_rows, HEADS, HEAD_DIM)

    queries = unit_rows(jax.nn.silu(by_head(query_pre))) * HEAD_DIM ** (-0.5)
    keys_unit = unit_rows(jax.nn.silu(by_head(key_pre)))
    values_act = jax.nn.silu(by_head(value_pre))
    strength = jax.nn.sigmoid(write_pre)
    retain = jnp.exp(-jnp.exp(decay_log) * jax.nn.softplus(decay_pre + decay_bias))
    recalled_values = jnp.einsum(
        "bhkv,bhk->bhv", old_state, keys_unit, precision=lax.Precision.HIGHEST
    )
    correction = values_act - retain[..., None] * recalled_values
    new_state = (
        retain[..., None, None] * old_state
        + (strength[..., None] * keys_unit)[..., :, None] * correction[..., None, :]
    )
    state_readout = jnp.einsum("bhkv,bhk->bhv", new_state, queries, precision=lax.Precision.HIGHEST)
    gated_read = (
        state_readout * norm_scale(state_readout) * head_gain * jax.nn.silu(by_head(outgate_pre))
    )
    gated_read = gated_read.reshape(local_rows, HEADS * HEAD_DIM).astype(jnp.bfloat16)
    read_cols = lax.all_to_all(gated_read, "kv", split_axis=1, concat_axis=0, tiled=True)
    partial_out = jnp.dot(read_cols, w_output, preferred_element_type=jnp.float32)
    mixer_out = lax.psum(partial_out, "kv")
    residual = lax.optimization_barrier((tok_wide + mixer_out).astype(jnp.bfloat16))
    residual_wide = residual.astype(jnp.float32)
    scale_mid = norm_scale(residual_wide)
    normed_mid = (residual_wide * channel_gain).astype(jnp.bfloat16)
    gate_act = jnp.dot(normed_mid, w_gate, preferred_element_type=jnp.float32) * scale_mid
    upward = jnp.dot(normed_mid, w_up, preferred_element_type=jnp.float32) * scale_mid
    own_residual = lax.dynamic_slice_in_dim(residual_wide, offset_cols, width_share, 1)
    hidden_units = (jax.nn.silu(gate_act) * upward).astype(jnp.bfloat16)
    down_sum = jnp.dot(
        lax.all_gather(hidden_units, "kv", axis=1, tiled=True),
        w_down,
        preferred_element_type=jnp.float32,
    )
    mixed = (own_residual + down_sum).astype(jnp.bfloat16)
    return (mixed, new_state)


TOKENS, PRE, READ, PARTIAL, RESIDUAL, HIDDEN = range(6)


def silu(values):
    return values / (1.0 + jnp.exp(-values))


def dot_rows(lhs, rows):
    return lax.dot_general(lhs, rows, (((1,), (1,)), ((), ())), preferred_element_type=F32)


def layer_kernel(
    n,
    depth_tile,
    tok_ref,
    mixer_gain_ref,
    decay_log_ref,
    decay_bias_ref,
    head_gain_ref,
    channel_gain_ref,
    w_query,
    w_key,
    w_value,
    w_outgate,
    w_decay,
    w_write,
    old_state,
    w_output,
    w_gate,
    w_up,
    w_down,
    mixed_ref,
    new_state,
    v_query,
    v_key,
    v_value,
    v_outgate,
    v_decay,
    v_write,
    v_state,
    v_output,
    v_gate,
    v_up,
    v_down,
    tok_all,
    normed,
    small,
    pre_out,
    pre_in,
    head_rows,
    head_vals,
    head_gate,
    read_rows,
    read_out,
    read_in,
    part_out,
    part_in,
    res_own,
    res_all,
    hid_own,
    hid_all,
    sem_proj,
    sem_small,
    sem_mix,
    sem_down,
    send_sem,
    recv_sem,
):
    me = lax.axis_index("kv")
    rows, share = tok_ref.shape
    local_rows, heads = v_state.shape[0], v_state.shape[1]
    width = n * share
    own_heads = share // HEAD_DIM
    hidden_share = v_gate.shape[0]
    steps = width // depth_tile

    barrier = pltpu.get_barrier_semaphore()
    for k in range(1, n):
        pl.semaphore_signal(
            barrier, inc=1, device_id={"kv": lax.rem(me + k, n)}, device_id_type=MESH
        )

    proj = ((w_query, v_query), (w_key, v_key), (w_value, v_value), (w_outgate, v_outgate))
    mix = ((w_gate, v_gate), (w_up, v_up))

    def tile_copy(pair, step, sem):
        part = pl.ds(pl.multiple_of(step * depth_tile, depth_tile), depth_tile)
        return pltpu.make_async_copy(pair[0].at[part], pair[1].at[part], sem)

    def proj_copy(which, step):
        return tile_copy(proj[which], step, sem_proj.at[step, which])

    def mix_copy(which, step):
        part = pl.ds(pl.multiple_of(step * depth_tile, depth_tile), depth_tile)
        return pltpu.make_async_copy(
            mix[which][0].at[:, part], mix[which][1].at[:, part], sem_mix.at[step, which]
        )

    def down_copy(step):
        part = pl.ds(pl.multiple_of(step * hidden_share, 16), hidden_share)
        return pltpu.make_async_copy(w_down.at[part], v_down.at[part], sem_down.at[step])

    decay_copy = pltpu.make_async_copy(w_decay, v_decay, sem_small.at[0])
    write_copy = pltpu.make_async_copy(w_write, v_write, sem_small.at[1])
    state_copy = pltpu.make_async_copy(old_state, v_state, sem_small.at[2])
    output_copy = pltpu.make_async_copy(w_output, v_output, sem_small.at[3])
    decay_copy.start()
    write_copy.start()
    for step in range(steps):
        for which in range(4):
            proj_copy(which, step).start()

    pl.semaphore_wait(barrier, n - 1)

    def exchange(phase, source, slots):
        copies = []
        for k in range(1, n):
            peer = lax.rem(me + k, n)
            copy = pltpu.make_async_remote_copy(
                src_ref=source(peer),
                dst_ref=slots.at[me],
                send_sem=send_sem.at[phase, k],
                recv_sem=recv_sem.at[phase, k],
                device_id={"kv": peer},
                device_id_type=MESH,
            )
            copy.start()
            copies.append(copy)
        return copies

    def arrive(copies):
        for copy in copies:
            copy.wait_recv()

    all_copies = []

    copies = exchange(TOKENS, lambda peer: tok_ref, tok_all)
    all_copies += copies
    state_copy.start()
    output_copy.start()
    for step in range(steps):
        for which in range(2):
            mix_copy(which, step).start()
    for step in range(n):
        down_copy(step).start()
    tok_all[me] = tok_ref[...]
    if pre_out.shape[1] > 4 * own_heads:
        pre_out[:, 4 * own_heads :, :] = jnp.zeros(
            (rows, pre_out.shape[1] - 4 * own_heads, HEAD_DIM), F32
        )
    read_out[...] = jnp.zeros_like(read_out)
    head_rows[...] = jnp.zeros_like(head_rows)
    arrive(copies)

    def norm_into(blocks, gain_ref):
        squares = jnp.zeros((rows, 1), F32)
        for s in range(n):
            cols = slice(s * share, (s + 1) * share)
            wide = blocks[s].astype(F32)
            squares += jnp.sum(wide * wide, axis=-1, keepdims=True)
            normed[:, cols] = (wide * gain_ref[:, cols]).astype(BF16)
        return lax.rsqrt(squares / width + EPS)

    scale_in = norm_into(tok_all, mixer_gain_ref)

    decay_copy.wait()
    write_copy.wait()

    def proj_step(step, sums):
        part = pl.ds(pl.multiple_of(step * depth_tile, depth_tile), depth_tile)
        lhs = normed[:, part]
        out = []
        for which in range(4):
            proj_copy(which, step).wait()
            out.append(
                sums[which]
                + jnp.dot(lhs, proj[which][1][part, :], preferred_element_type=F32)
            )
        out.append(sums[4] + dot_rows(lhs, v_decay[:, part]))
        out.append(sums[5] + dot_rows(lhs, v_write[:, part]))
        return tuple(out)

    zeros = lambda cols: jnp.zeros((rows, cols), F32)
    sums = lax.fori_loop(
        0, steps, proj_step, (zeros(share),) * 4 + (zeros(heads),) * 2
    )
    for which in range(4):
        pre = (sums[which] * scale_in).astype(BF16).astype(F32)
        for j in range(own_heads):
            pre_out[:, which * own_heads + j, :] = pre[:, j * HEAD_DIM : (j + 1) * HEAD_DIM]

    def row_block(peer):
        return pre_out.at[pl.ds(peer * local_rows, local_rows)]

    copies = exchange(PRE, row_block, pre_in)
    all_copies += copies
    pre_in[me] = pre_out[pl.ds(me * local_rows, local_rows)]
    small[0] = sums[4] * scale_in
    small[1] = sums[5] * scale_in
    state_copy.wait()
    arrive(copies)

    for l in range(local_rows):
        own = pl.ds(me * local_rows + l, 1)
        decay_pre = small[0, own, :]
        write_pre = small[1, own, :]
        strength = 1.0 / (1.0 + jnp.exp(-write_pre))
        shifted = decay_pre + decay_bias_ref[...]
        softplus = jnp.maximum(shifted, 0.0) + jnp.log1p(jnp.exp(-jnp.abs(shifted)))
        retain = jnp.exp(-jnp.exp(decay_log_ref[...]) * softplus)
        for s in range(n):
            act = silu(pre_in[s, l])
            unit = act * lax.rsqrt(jnp.sum(act * act, axis=-1, keepdims=True) + EPS)
            at = s * own_heads
            c = own_heads
            head_rows[at : at + c, :] = unit[c : 2 * c]
            head_rows[heads + at : heads + at + c, :] = unit[:c] * HEAD_DIM ** (-0.5)
            head_vals[at : at + c, :] = act[2 * c : 3 * c]
            head_gate[at : at + c, :] = act[3 * c : 4 * c]
        columns = head_rows[...].T
        for h in range(heads):
            key = columns[:, h : h + 1]
            query = columns[:, heads + h : heads + h + 1]
            keep = retain[:, h : h + 1]
            old = v_state[l, h]
            recalled = jnp.sum(old * key, axis=0, keepdims=True)
            correction = head_vals[h : h + 1, :] - keep * recalled
            new = keep * old + key * (strength[:, h : h + 1] * correction)
            v_state[l, h] = new
            read_rows[h : h + 1, :] = jnp.sum(new * query, axis=0, keepdims=True)
        read = read_rows[...]
        scale = lax.rsqrt(jnp.mean(read * read, axis=-1, keepdims=True) + EPS)
        gated = (read * scale * head_gain_ref[...] * head_gate[...]).astype(BF16).astype(F32)
        for s in range(n):
            read_out[s, l, :own_heads, :] = gated[s * own_heads : (s + 1) * own_heads]

    copies = exchange(READ, lambda peer: read_out.at[peer], read_in)
    all_copies += copies
    state_out = pltpu.make_async_copy(v_state, new_state, sem_small.at[4])
    state_out.start()
    read_in[me] = read_out[me]
    output_copy.wait()
    arrive(copies)
    read_cols = jnp.concatenate(
        [read_in[:, :, j, :].reshape(rows, HEAD_DIM) for j in range(own_heads)], axis=1
    ).astype(BF16)
    for s in range(n):
        part_out[s] = jnp.dot(
            read_cols, v_output[:, s * share : (s + 1) * share], preferred_element_type=F32
        )

    copies = exchange(PARTIAL, lambda peer: part_out.at[peer], part_in)
    all_copies += copies
    part_in[me] = part_out[me]
    arrive(copies)
    residual = tok_ref[...].astype(F32)
    mixer = part_in[0]
    for s in range(1, n):
        mixer += part_in[s]
    res_own[...] = (residual + mixer).astype(BF16)
    copies = exchange(RESIDUAL, lambda peer: res_own, res_all)
    all_copies += copies
    res_all[me] = res_own[...]
    arrive(copies)
    scale_mid = norm_into(res_all, channel_gain_ref)

    def mix_step(step, sums):
        part = pl.ds(pl.multiple_of(step * depth_tile, depth_tile), depth_tile)
        lhs = normed[:, part]
        out = []
        for which in range(2):
            mix_copy(which, step).wait()
            out.append(
                sums[which] + dot_rows(lhs, mix[which][1][:, part])
            )
        return tuple(out)

    gate, up = lax.fori_loop(0, steps, mix_step, (zeros(hidden_share),) * 2)
    hid_own[...] = (silu(gate * scale_mid) * (up * scale_mid)).astype(BF16)

    copies = exchange(HIDDEN, lambda peer: hid_own, hid_all)
    all_copies += copies
    hid_all[me] = hid_own[...]
    arrive(copies)

    def down_step(step, total):
        down_copy(step).wait()
        part = pl.ds(pl.multiple_of(step * hidden_share, 16), hidden_share)
        return total + jnp.dot(hid_all[step], v_down[part, :], preferred_element_type=F32)

    total = lax.fori_loop(0, n, down_step, zeros(share))
    mixed_ref[...] = (res_own[...].astype(F32) + total).astype(BF16)

    for copy in all_copies:
        copy.wait_send()
    state_out.wait()


def round_up(value, unit):
    return -(-value // unit) * unit


def fused_body(
    n,
    tokens,
    old_state,
    mixer_gain,
    w_query,
    w_key,
    w_value,
    w_outgate,
    w_decay,
    w_write,
    decay_log,
    decay_bias,
    head_gain,
    w_output,
    channel_gain,
    w_gate,
    w_up,
    w_down,
):
    rows, share = tokens.shape
    local_rows, heads = old_state.shape[:2]
    width, hidden_share = w_gate.shape
    own_heads = share // HEAD_DIM
    depth_tile = 512 if width % 512 == 0 else share
    steps = width // depth_tile
    pre_rows = round_up(4 * own_heads, 8)
    read_slots = round_up(own_heads, 8)
    vmem = pl.BlockSpec(memory_space=pltpu.VMEM)
    hbm = pl.BlockSpec(memory_space=pl.ANY)
    buf = pltpu.VMEM
    sem = pltpu.SemaphoreType.DMA
    wide = lambda vector: vector.reshape(1, -1)
    return tuple(
        pl.pallas_call(
            functools.partial(layer_kernel, n, depth_tile),
            out_shape=(
                jax.ShapeDtypeStruct((rows, share), BF16),
                jax.ShapeDtypeStruct(old_state.shape, F32),
            ),
            in_specs=[vmem] * 6 + [hbm] * 11,
            out_specs=(vmem, hbm),
            scratch_shapes=[
                buf((width, share), BF16),
                buf((width, share), BF16),
                buf((width, share), BF16),
                buf((width, share), BF16),
                buf((heads, width), BF16),
                buf((heads, width), BF16),
                buf(old_state.shape, F32),
                buf(w_output.shape, BF16),
                buf((hidden_share, width), BF16),
                buf((hidden_share, width), BF16),
                buf(w_down.shape, BF16),
                buf((n, rows, share), BF16),
                buf((rows, width), BF16),
                buf((2, rows, heads), F32),
                buf((rows, pre_rows, HEAD_DIM), F32),
                buf((n, local_rows, pre_rows, HEAD_DIM), F32),
                buf((round_up(2 * heads, 128), HEAD_DIM), F32),
                buf((heads, HEAD_DIM), F32),
                buf((heads, HEAD_DIM), F32),
                buf((heads, HEAD_DIM), F32),
                buf((n, local_rows, read_slots, HEAD_DIM), F32),
                buf((n, local_rows, read_slots, HEAD_DIM), F32),
                buf((n, rows, share), F32),
                buf((n, rows, share), F32),
                buf((rows, share), BF16),
                buf((n, rows, share), BF16),
                buf((rows, hidden_share), BF16),
                buf((n, rows, hidden_share), BF16),
                sem((steps, 4)),
                sem((5,)),
                sem((steps, 2)),
                sem((n,)),
                sem((6, n)),
                sem((6, n)),
            ],
            compiler_params=pltpu.CompilerParams(
                collective_id=0, has_side_effects=True, vmem_limit_bytes=63 * 2**20
            ),
        )(
            tokens,
            wide(mixer_gain),
            wide(decay_log),
            wide(decay_bias),
            wide(head_gain),
            wide(channel_gain),
            w_query,
            w_key,
            w_value,
            w_outgate,
            w_decay.T,
            w_write.T,
            old_state,
            w_output,
            w_gate.T,
            w_up.T,
            w_down,
        )
    )


def any_body(n, tokens, old_state, *rest):
    whole_heads = tokens.shape[1] % HEAD_DIM == 0 and tokens.shape[0] % 8 == 0
    held = sum(a.size * a.dtype.itemsize for a in (old_state, *rest))
    if whole_heads and held < 40 * 2**20:
        return fused_body(n, tokens, old_state, *rest)
    return body(tokens, old_state, *rest)


def solution(mesh):
    in_specs = (
        P(("tp", "dp"), "kv"),
        P(("tp", "dp", "kv"), None, None, None),
        P(),
        P(None, "kv"),
        P(None, "kv"),
        P(None, "kv"),
        P(None, "kv"),
        P(),
        P(),
        P(),
        P(),
        P(),
        P("kv", None),
        P(),
        P(None, "kv"),
        P(None, "kv"),
        P(None, "kv"),
    )
    out_specs = (P(("tp", "dp"), "kv"), P(("tp", "dp", "kv"), None, None, None))
    return jax.shard_map(
        functools.partial(any_body, mesh.shape["kv"]), mesh=mesh, in_specs=in_specs, out_specs=out_specs, check_vma=False)
```
